32 devices in a mesh: sp: 4 (over y, x), tp: 8 (over z, core).
Axes of the slice: x: 2, y: 2, z: 4, core: 2. Of those that a mesh axis runs over, the one named last changes fastest.
Arguments:
- residual: bfloat16 [4096, 2048], P(('sp', 'tp')), may hold values from -6 to 6
- wide_query: bfloat16 [4096, 1024], P('sp', 'tp'), may hold values from -8 to 8
- narrow_query: bfloat16 [4096, 1024], P('sp', 'tp'), may hold values from -8 to 8
- wide_keys: bfloat16 [4096, 256], P('sp'), may hold values from -6 to 6
- narrow_keys: bfloat16 [4096, 256], P('sp'), may hold values from -6 to 6
- wide_values: bfloat16 [4096, 256], P('sp'), may hold values from -6 to 6
- narrow_values: bfloat16 [4096, 256], P('sp'), may hold values from -6 to 6
- wide_query_gain: float32 [64], replicated, may hold values from 1.2 to 10
- wide_key_gain: float32 [64], replicated, may hold values from 1.2 to 10
- narrow_query_gain: float32 [32], replicated, may hold values from 1.2 to 10
- narrow_key_gain: float32 [32], replicated, may hold values from 1.2 to 10
- wide_out: bfloat16 [1024, 2048], P('tp'), may hold values from -0.25 to 0.25
- narrow_out: bfloat16 [1024, 2048], P('tp'), may hold values from -0.25 to 0.25
- first_gain: float32 [2048], replicated, may hold values from 0.1 to 1.9
- first_bias: float32 [2048], replicated, may hold values from -1.8 to 1.8
- route_ids: int32 [4096, 2], P(('sp', 'tp')), may hold values from 0 to 7, all different within a row; in each aligned block of 128 rows (0 to 127, 128 to 255, ...) at most 40 rows name the same one
- route_weights: float32 [4096, 2], P(('sp', 'tp')), may hold values from 0.25 to 2.5
- expert_gate: bfloat16 [8, 2048, 3072], P('sp', None, 'tp'), may hold values from -0.125 to 0.125
- expert_up: bfloat16 [8, 2048, 3072], P('sp', None, 'tp'), may hold values from -0.125 to 0.125
- expert_down: bfloat16 [8, 3072, 2048], P('sp', 'tp'), may hold values from -0.109375 to 0.109375
- shared_gate: bfloat16 [2048, 256], replicated, may hold values from -0.125 to 0.125
- shared_up: bfloat16 [2048, 256], replicated, may hold values from -0.125 to 0.125
- shared_down: bfloat16 [256, 2048], replicated, may hold values from -0.375 to 0.375
- second_gain: float32 [2048], replicated, may hold values from 0.1 to 1.9
- second_bias: float32 [2048], replicated, may hold values from -1.8 to 1.8
Outputs:
- layer_output: bfloat16 [4096, 2048], P(('sp', 'tp'))
The draws below stay inside these ranges and needn't reach their ends.
Inputs may be any that keep to these rules, and one draw needn't show every extreme that they name: `route_ids`: each row names 2 different experts. The rows of one device (aligned blocks of 128 rows) name each expert at most 40 times, and in every draw some expert is named exactly 40 times in the rows of some device.
All inputs are finite; a program needn't handle non-finite values.
Results may differ from the reference program's by a relative error of at most 0.02.
The reference program's roundings to bfloat16 on the way count: a program that leaves them out, or rounds other values in their place, can miss the bound.
Values may be sent and summed in bfloat16 or wider, within the bound.
A program may use at most 128 MiB of HBM per device.

```python
import math
import jax
import jax.numpy as jnp
import numpy as np
from jax import lax

MODEL_WIDTH = 2048
WIDE_HEADS = 16
WIDE_SIZE = 64
WIDE_GROUPS = 4
NARROW_HEADS = 32
NARROW_SIZE = 32
NARROW_GROUPS = 8
GRID_WIDTH = 64
EXPERT_WIDTH = 3072
SHARED_WIDTH = 256
ROUTE_TOP = 2
SEQ_TOKENS = 4096
TOKENS = 4096
DEVICE_ROWS = 128
EXPERTS = 8
CAPACITY = 40
N_SP = 4
N_TP = 8


def gain_pair(key, head_size, salt):
    folded = jax.random.fold_in(key, salt)
    draw_one = jax.random.uniform(jax.random.fold_in(folded, 2), (head_size,), jnp.float32)
    draw_two = jax.random.uniform(jax.random.fold_in(folded, 3), (head_size,), jnp.float32)
    query_gain = 1.5 * 2.0 ** draw_one
    key_gain = 1.5 * 2.0 ** draw_two
    return (query_gain, key_gain)


def field(key, heads, head_size, salt):
    folded = jax.random.fold_in(key, salt)
    return jnp.clip(jax.random.normal(folded, (TOKENS, heads, head_size), jnp.float32), -6.0, 6.0)


def drawn_queries(key, heads, head_size, salt):
    values = field(key, heads, head_size, salt + 100)
    return values.reshape(TOKENS, heads * head_size).astype(jnp.bfloat16)


def drawn_keys(key, heads, head_size, salt):
    values = field(key, heads, head_size, salt + 300)
    return values.reshape(TOKENS, heads * head_size).astype(jnp.bfloat16)


def draw_wide_query(key, part):
    return drawn_queries(key, WIDE_HEADS, WIDE_SIZE, 11)


def draw_narrow_query(key, part):
    return drawn_queries(key, NARROW_HEADS, NARROW_SIZE, 23)


def draw_wide_keys(key, part):
    return drawn_keys(key, WIDE_GROUPS, WIDE_SIZE, 11)


def draw_narrow_keys(key, part):
    return drawn_keys(key, NARROW_GROUPS, NARROW_SIZE, 23)


def draw_wide_query_gain(key, part):
    return gain_pair(key, WIDE_SIZE, 11)[0]


def draw_wide_key_gain(key, part):
    return gain_pair(key, WIDE_SIZE, 11)[1]


def draw_narrow_query_gain(key, part):
    return gain_pair(key, NARROW_SIZE, 23)[0]


def draw_narrow_key_gain(key, part):
    return gain_pair(key, NARROW_SIZE, 23)[1]


def levels(own_key, extent, shards, smallest, top_value):
    factor_of, own = 1.0, jax.random.fold_in(own_key, 6)
    for dim, parts in shards:
        heights = jnp.exp(jax.random.uniform(jax.random.fold_in(own, dim), (parts,), jnp.float32, smallest / len(shards), top_value / len(shards)))
        factor_of = factor_of * jnp.repeat(heights, extent[dim] // parts).reshape([-1 if axis == dim else 1 for axis in range(len(extent))])
    return factor_of


def shared_out(own_key, own, number, rows, number_of, top, bound, slope):
    ranking = jax.random.permutation(own_key, number_of)
    packed, usual = shares(number_of, rows * top, bound, slope, True), shares(number_of, rows * top, bound, slope, False)
    places = jnp.arange(number_of)

    def named(sizes, rotation):
        used = int((sizes > 0).sum())
        fixed = max(1, used // 4)
        passed = fixed + (places - fixed + rotation * (used - fixed)) % max(1, number_of - fixed)
        return jnp.zeros((number_of,), jnp.int32).at[ranking[jnp.where(places < fixed, places, passed)]].set(jnp.asarray(sizes, jnp.int32))

    sizes = jnp.where(number % 4 == 0, named(packed, number // 4), named(usual, number - number // 4 - 1))
    mixed = jax.random.permutation(jax.random.fold_in(own, 3), number_of)
    giver, sink = mixed[0:number_of // 2 * 2:2], mixed[1:number_of // 2 * 2:2]
    room = jnp.minimum(sizes[giver] - 1, bound - sizes[sink]) // 2
    room = jnp.where((giver == ranking[0]) | (sink == ranking[0]) | (sizes[sink] == 0), 0, jnp.maximum(room, 0))
    passed = jax.random.randint(jax.random.fold_in(own, 4), (number_of // 2,), 0, 1 << 20) % (room + 1)
    sizes = sizes.at[giver].add(-passed).at[sink].add(passed)
    items = jnp.searchsorted(jnp.cumsum(sizes), jnp.arange(rows * top), side="right").astype(jnp.int32)
    table = items.reshape(top, rows).T
    table = table[jax.random.permutation(jax.random.fold_in(own, 1), rows)]
    rotation = jax.random.randint(jax.random.fold_in(own, 2), (rows, 1), 0, top)
    return jnp.take_along_axis(table, (jnp.arange(top)[None, :] + rotation) % top, axis=1)


def shares(number_of, total, most, lean, full):
    weights = [(1 << 20) // math.isqrt(rank ** lean) + 1 for rank in range(1, number_of + 1)]
    largest = most if full else min(most, max(-(-total // number_of), total * weights[0] // sum(weights)))
    least = 1 if total - largest >= number_of - 1 else 0
    given, surplus = [largest] + [least] * (number_of - 1), total - largest - least * (number_of - 1)
    while surplus > 0:
        movable = [i for i in range(1, number_of) if given[i] < largest] or [i for i in range(1, number_of) if given[i] < most]
        pool, left = sum([weights[i] for i in movable]), surplus
        for i in movable:
            more = min(most - given[i], max(1, left * weights[i] // pool), surplus)
            given[i] = given[i] + more
            surplus = surplus - more
    return np.array(given)


def gaussian(rng, shape, scale, limit, cuts=(), kind=jnp.bfloat16):
    values = jax.random.normal(rng, shape, jnp.float32) * scale
    if len(cuts) > 0:
        values = levels(rng, shape, cuts, -0.22, 0.18) * values
    return jnp.clip(values, min=-limit, max=limit).astype(kind)


def setup_inputs(seed: int = 0) -> dict:
    streams_of = jax.random.split(jax.random.key(seed), 26)
    residual = gaussian(streams_of[0], (TOKENS, MODEL_WIDTH), 1.0, 6.0, ((0, 32),))
    wide_query = draw_wide_query(jax.random.fold_in(streams_of[25], 71), 0)
    narrow_query = draw_narrow_query(jax.random.fold_in(streams_of[25], 71), 0)
    wide_keys = draw_wide_keys(jax.random.fold_in(streams_of[25], 71), 0)
    narrow_keys = draw_narrow_keys(jax.random.fold_in(streams_of[25], 71), 0)
    wide_values = gaussian(streams_of[5], (TOKENS, WIDE_GROUPS * WIDE_SIZE), 1.0, 6.0, ((0, 4),))
    narrow_values = gaussian(streams_of[6], (TOKENS, NARROW_GROUPS * NARROW_SIZE), 1.0, 6.0, ((0, 4),))
    wide_query_gain = draw_wide_query_gain(jax.random.fold_in(streams_of[25], 71), 0)
    wide_key_gain = draw_wide_key_gain(jax.random.fold_in(streams_of[25], 71), 0)
    narrow_query_gain = draw_narrow_query_gain(jax.random.fold_in(streams_of[25], 71), 0)
    narrow_key_gain = draw_narrow_key_gain(jax.random.fold_in(streams_of[25], 71), 0)
    wide_out = gaussian(streams_of[11], (WIDE_HEADS * WIDE_SIZE, MODEL_WIDTH), (WIDE_HEADS * WIDE_SIZE // 2) ** -0.5, 0.25, ((0, 8),))
    narrow_out = gaussian(streams_of[12], (NARROW_HEADS * NARROW_SIZE, MODEL_WIDTH), (NARROW_HEADS * NARROW_SIZE // 2) ** -0.5, 0.25, ((0, 8),))
    first_gain = jnp.clip(1.0 + 0.18 * jax.random.normal(streams_of[13], (MODEL_WIDTH,), jnp.float32), 0.1, 1.9)
    first_bias = gaussian(streams_of[14], (MODEL_WIDTH,), 0.3, 1.8, (), jnp.float32)
    route_ids_keys = jax.random.split(jax.random.fold_in(streams_of[15], 1), TOKENS // DEVICE_ROWS)
    route_ids_turns = jax.random.permutation(jax.random.fold_in(streams_of[15], 3), TOKENS // DEVICE_ROWS)
    route_ids = jax.vmap(lambda own, number: shared_out(jax.random.fold_in(streams_of[15], 2), own, number, DEVICE_ROWS, EXPERTS, ROUTE_TOP, CAPACITY, 2))(route_ids_keys, route_ids_turns).reshape((TOKENS, ROUTE_TOP))
    route_weights = jnp.clip(jnp.exp(math.log(2.5) - 2.3025851 * jax.random.uniform(streams_of[16], (TOKENS, ROUTE_TOP), jnp.float32) ** levels(streams_of[16], (TOKENS, ROUTE_TOP), ((0, 32),), -0.2, 0.2)), 0.25, 2.5)
    expert_gate = gaussian(streams_of[17], (EXPERTS, MODEL_WIDTH, EXPERT_WIDTH), MODEL_WIDTH ** -0.5, 0.125, ((0, 4), (2, 8)))
    expert_up = gaussian(streams_of[18], (EXPERTS, MODEL_WIDTH, EXPERT_WIDTH), MODEL_WIDTH ** -0.5, 0.125, ((0, 4), (2, 8)))
    expert_down = gaussian(streams_of[19], (EXPERTS, EXPERT_WIDTH, MODEL_WIDTH), EXPERT_WIDTH ** -0.5, 0.109375, ((0, 4), (1, 8)))
    shared_gate = gaussian(streams_of[20], (MODEL_WIDTH, SHARED_WIDTH), MODEL_WIDTH ** -0.5, 0.125)
    shared_up = gaussian(streams_of[21], (MODEL_WIDTH, SHARED_WIDTH), MODEL_WIDTH ** -0.5, 0.125)
    shared_down = gaussian(streams_of[22], (SHARED_WIDTH, MODEL_WIDTH), SHARED_WIDTH ** -0.5, 0.375)
    second_gain = jnp.clip(1.0 + 0.18 * jax.random.normal(streams_of[23], (MODEL_WIDTH,), jnp.float32), 0.1, 1.9)
    second_bias = gaussian(streams_of[24], (MODEL_WIDTH,), 0.3, 1.8, (), jnp.float32)
    return {"residual": residual, "wide_query": wide_query, "narrow_query": narrow_query, "wide_keys": wide_keys, "narrow_keys": narrow_keys, "wide_values": wide_values, "narrow_values": narrow_values, "wide_query_gain": wide_query_gain, "wide_key_gain": wide_key_gain, "narrow_query_gain": narrow_query_gain, "narrow_key_gain": narrow_key_gain, "wide_out": wide_out, "narrow_out": narrow_out, "first_gain": first_gain, "first_bias": first_bias, "route_ids": route_ids, "route_weights": route_weights, "expert_gate": expert_gate, "expert_up": expert_up, "expert_down": expert_down, "shared_gate": shared_gate, "shared_up": shared_up, "shared_down": shared_down, "second_gain": second_gain, "second_bias": second_bias}


EPS_HEAD = 1e-06
EPS_LAYER = 1e-05
ALPHA = 2.0 ** 0.25
THETA = 10000.0

def head_norm(values, gain_vec):
    mean_square = lax.optimization_barrier(jnp.mean(values * values, axis=-1, keepdims=True))
    return values * lax.rsqrt(mean_square + EPS_HEAD) * gain_vec

def rotate(values, position):
    half_size = values.shape[-1] // 2
    frequency = THETA ** (-jnp.arange(half_size, dtype=jnp.float32) / half_size)
    angles = position.astype(jnp.float32)[:, None] * frequency
    cosine = jnp.cos(angles)[:, None, :]
    sine_part = jnp.sin(angles)[:, None, :]
    leading = values[..., :half_size]
    trailing = values[..., half_size:]
    return jnp.concatenate([leading * cosine - trailing * sine_part, trailing * cosine + leading * sine_part], axis=-1)

def grid_rotate(values, position):
    half_size = values.shape[-1] // 2
    grid_row = position // GRID_WIDTH
    grid_col = position % GRID_WIDTH
    return jnp.concatenate([rotate(values[..., :half_size], grid_row), rotate(values[..., half_size:], grid_col)], axis=-1)

def layer_norm(values, gain_vec, bias_vec):
    center = lax.optimization_barrier(jnp.mean(values, axis=-1, keepdims=True))
    shifted = values - center
    variance = lax.optimization_barrier(jnp.mean(shifted * shifted, axis=-1, keepdims=True))
    return (shifted * lax.rsqrt(variance + EPS_LAYER) * gain_vec + bias_vec).astype(jnp.bfloat16)

def attend_group(queries, keys_all, values_all, query_gain, key_gain, heads_total, groups):
    head_size = query_gain.shape[0]
    per_group = heads_total // groups
    seq_count = TOKENS // SEQ_TOKENS
    block_rows = min(512, SEQ_TOKENS)
    position = jnp.arange(SEQ_TOKENS, dtype=jnp.int32)
    score_scale = head_size ** (-0.5)
    query_seq = queries.reshape(seq_count, SEQ_TOKENS, heads_total, head_size)
    key_seq = keys_all.reshape(seq_count, SEQ_TOKENS, groups, head_size)
    value_seq = values_all.reshape(seq_count, SEQ_TOKENS, groups, head_size)

    def one_sequence(operands):
        query_rows, key_rows, value_rows = operands
        rotated_queries = grid_rotate(head_norm(query_rows.astype(jnp.float32), query_gain), position).astype(jnp.bfloat16)
        rotated_keys = grid_rotate(head_norm(key_rows.astype(jnp.float32), key_gain), position).astype(jnp.bfloat16)
        key_float = rotated_keys.astype(jnp.float32)
        value_float = value_rows.astype(jnp.float32)
        blocks = rotated_queries.reshape(SEQ_TOKENS // block_rows, block_rows, groups, per_group, head_size)

        def one_block(query_block):
            scores = jnp.einsum('qgpd,kgd->gpqk', query_block.astype(jnp.float32), key_float) * score_scale
            largest = lax.optimization_barrier(jnp.max(scores, axis=-1, keepdims=True))
            weights = jnp.exp(scores - largest)
            weights = (weights / lax.optimization_barrier(jnp.sum(weights, axis=-1, keepdims=True))).astype(jnp.bfloat16)
            mixed_rows = jnp.einsum('gpqk,kgd->qgpd', weights.astype(jnp.float32), value_float)
            return mixed_rows.astype(jnp.bfloat16)
        mixed_all = lax.map(one_block, blocks)
        return mixed_all.reshape(SEQ_TOKENS, heads_total * head_size)
    result = lax.map(one_sequence, (query_seq, key_seq, value_seq))
    return result.reshape(TOKENS, heads_total * head_size)

def routed_sum(hidden, route_ids, route_weights, expert_gate, expert_up, expert_down):
    assignments = TOKENS * ROUTE_TOP
    most = N_SP * N_TP * CAPACITY
    flat_ids = route_ids.reshape(-1).astype(jnp.int32)
    order = jnp.argsort(flat_ids, stable=True).astype(jnp.int32)
    counts = lax.optimization_barrier(jnp.sum((flat_ids[:, None] == jnp.arange(EXPERTS, dtype=jnp.int32)[None, :]).astype(jnp.int32), axis=0))
    starts = jnp.cumsum(counts) - counts
    slot_rank = jnp.arange(most, dtype=jnp.int32)
    position_in = (starts[:, None] + slot_rank[None, :]).astype(jnp.int32)
    valid = slot_rank[None, :] < counts[:, None]
    picked = jnp.where(valid, order[jnp.minimum(position_in, assignments - 1)], assignments).astype(jnp.int32)
    token_rows = (picked // ROUTE_TOP).astype(jnp.int32)
    padded_hidden = jnp.concatenate([hidden, jnp.zeros((1, MODEL_WIDTH), jnp.bfloat16)], axis=0)
    block_width = EXPERT_WIDTH // N_TP

    def one_expert(operands):
        rows_index, gate_weight, up_weight, down_weight = operands
        rows_in = padded_hidden[rows_index]
        gate_values = jnp.dot(rows_in, gate_weight, preferred_element_type=jnp.float32)
        up_values = jnp.dot(rows_in, up_weight, preferred_element_type=jnp.float32)
        active = (jax.nn.silu(gate_values) * up_values).astype(jnp.bfloat16)
        blocks_in = active.reshape(most, N_TP, block_width).astype(jnp.float32)
        down_blocks = down_weight.reshape(N_TP, block_width, MODEL_WIDTH).astype(jnp.float32)
        partial_value = lax.optimization_barrier(jnp.einsum('mtf,tfd->tmd', blocks_in, down_blocks).astype(jnp.bfloat16))
        return lax.optimization_barrier(jnp.sum(partial_value.astype(jnp.float32), axis=0)).astype(jnp.bfloat16)
    outputs = lax.map(one_expert, (token_rows, expert_gate, expert_up, expert_down))
    padded_weights = jnp.concatenate([route_weights.reshape(-1), jnp.zeros((1,), jnp.float32)], axis=0)
    slot_weight = padded_weights[picked]
    contribution = slot_weight[:, :, None] * outputs.astype(jnp.float32)
    total = jnp.zeros((TOKENS + 1, MODEL_WIDTH), jnp.float32).at[token_rows.reshape(-1)].add(contribution.reshape(-1, MODEL_WIDTH))
    return total[:TOKENS]

def reference(residual, wide_query, narrow_query, wide_keys, narrow_keys, wide_values, narrow_values, wide_query_gain, wide_key_gain, narrow_query_gain, narrow_key_gain, wide_out, narrow_out, first_gain, first_bias, route_ids, route_weights, expert_gate, expert_up, expert_down, shared_gate, shared_up, shared_down, second_gain, second_bias):
    wide_mixed = attend_group(wide_query, wide_keys, wide_values, wide_query_gain, wide_key_gain, WIDE_HEADS, WIDE_GROUPS)
    narrow_mixed = attend_group(narrow_query, narrow_keys, narrow_values, narrow_query_gain, narrow_key_gain, NARROW_HEADS, NARROW_GROUPS)
    projected = jnp.dot(wide_mixed, wide_out, preferred_element_type=jnp.float32) + jnp.dot(narrow_mixed, narrow_out, preferred_element_type=jnp.float32)
    hidden = layer_norm(ALPHA * residual.astype(jnp.float32) + projected, first_gain, first_bias)
    routed = routed_sum(hidden, route_ids, route_weights, expert_gate, expert_up, expert_down)
    shared_gate_values = jnp.dot(hidden, shared_gate, preferred_element_type=jnp.float32)
    shared_up_values = jnp.dot(hidden, shared_up, preferred_element_type=jnp.float32)
    shared_active = (jax.nn.silu(shared_gate_values) * shared_up_values).astype(jnp.bfloat16)
    shared_output = jnp.dot(shared_active, shared_down, preferred_element_type=jnp.float32)
    return layer_norm(ALPHA * hidden.astype(jnp.float32) + routed + shared_output, second_gain, second_bias)
```

```python
import functools
import math

import jax
import jax.numpy as jnp
from jax import lax
from jax.experimental import pallas as pl
from jax.experimental.pallas import tpu as pltpu
from jax.sharding import PartitionSpec as P

WIDE_HEADS = 16
WIDE_GROUPS = 4
NARROW_HEADS = 32
NARROW_GROUPS = 8
GRID_WIDTH = 64
SEQ_SHARDS = 4
LOCAL_EXPERTS = 2


EPS_HEAD = 1e-06
EPS_LAYER = 1e-05
ALPHA = 2.0**0.25
THETA = 10000.0


def swapped(x, axis, apart):
    return lax.ppermute(x, axis, [(i, i ^ 1 << apart) for i in range(lax.axis_size(axis))])


def head_norm(values, gain_vec):
    mean_square = jnp.mean(values * values, axis=-1, keepdims=True)
    return values * lax.rsqrt(mean_square + EPS_HEAD) * gain_vec


def rotate(values, position):
    half_size = values.shape[-1] // 2
    frequency = THETA ** (-jnp.arange(half_size, dtype=jnp.float32) / half_size)
    angles = position.astype(jnp.float32)[:, None] * frequency
    cosine = jnp.cos(angles)[:, None, :]
    sine_part = jnp.sin(angles)[:, None, :]
    leading = values[..., :half_size]
    trailing = values[..., half_size:]
    return jnp.concatenate(
        [leading * cosine - trailing * sine_part, trailing * cosine + leading * sine_part], axis=-1
    )


def grid_rotate(values, position):
    half_size = values.shape[-1] // 2
    grid_row = position // GRID_WIDTH
    grid_col = position % GRID_WIDTH
    return jnp.concatenate(
        [rotate(values[..., :half_size], grid_row), rotate(values[..., half_size:], grid_col)],
        axis=-1,
    )


def layer_norm(values, gain_vec, bias_vec):
    center = jnp.mean(values, axis=-1, keepdims=True)
    shifted = values - center
    variance = jnp.mean(shifted * shifted, axis=-1, keepdims=True)
    return (shifted * lax.rsqrt(variance + EPS_LAYER) * gain_vec + bias_vec).astype(jnp.bfloat16)


def prepare(queries, key_block, value_block, query_gain, key_gain, heads_total, groups, position):
    head_size = query_gain.shape[0]
    local_heads = queries.shape[1] // head_size
    group_index = lax.axis_index("tp") * local_heads // (heads_total // groups)
    query_rows = queries.reshape(queries.shape[0], local_heads, head_size).astype(jnp.float32)
    rotated_queries = grid_rotate(head_norm(query_rows, query_gain), position).astype(jnp.bfloat16)
    column_start = group_index * head_size
    key_rows = lax.dynamic_slice_in_dim(key_block, column_start, head_size, 1).astype(jnp.float32)[
        :, None, :
    ]
    rotated_keys = grid_rotate(head_norm(key_rows, key_gain), position)[:, 0, :].astype(
        jnp.bfloat16
    )
    value_rows = lax.dynamic_slice_in_dim(value_block, column_start, head_size, 1)
    return (rotated_queries, jnp.concatenate([rotated_keys, value_rows], axis=1))


def attend_kernel(query_ref, key_ref, value_ref, mixed_ref, *, factor):
    head_size = query_ref.shape[1]
    scores = lax.dot_general(
        query_ref[...], key_ref[...], (((1,), (1,)), ((), ())), preferred_element_type=jnp.float32
    )
    largest = jnp.max(scores, axis=-1, keepdims=True)
    weights = jnp.exp2((scores - largest) * factor).astype(jnp.bfloat16)
    sums = jnp.dot(weights, value_ref[...], preferred_element_type=jnp.float32)
    mixed_ref[...] = (sums[:, :head_size] / sums[:, head_size : head_size + 1]).astype(jnp.bfloat16)


def attend_local(rotated_queries, key_block, value_block, block_rows=256):
    seg_rows, local_heads, head_size = rotated_queries.shape
    keys = key_block.shape[0]
    rows = seg_rows * local_heads
    block_rows = min(block_rows, rows)
    value_ones = jnp.concatenate(
        [value_block, jnp.ones((keys, 128 - head_size), value_block.dtype)], axis=1
    )
    mixed_rows = pl.pallas_call(
        functools.partial(attend_kernel, factor=math.log2(math.e) * head_size ** (-0.5)),
        out_shape=jax.ShapeDtypeStruct((rows, head_size), jnp.bfloat16),
        grid=(rows // block_rows,),
        in_specs=[
            pl.BlockSpec((block_rows, head_size), lambda i: (i, 0)),
            pl.BlockSpec((keys, head_size), lambda i: (0, 0)),
            pl.BlockSpec((keys, 128), lambda i: (0, 0)),
        ],
        out_specs=pl.BlockSpec((block_rows, head_size), lambda i: (i, 0)),
        cost_estimate=pl.CostEstimate(
            flops=1024 * rows * keys, bytes_accessed=4 * rows * head_size, transcendentals=rows * keys
        ),
        compiler_params=pltpu.CompilerParams(vmem_limit_bytes=60 * 1024 * 1024),
    )(rotated_queries.reshape(rows, head_size), key_block, value_ones)
    return mixed_rows.reshape(seg_rows, local_heads * head_size)


def hop(x, step):
    tp_size = lax.axis_size("tp")
    if step == 0:
        pairs = [(i, i ^ 1) for i in range(tp_size)]
    else:
        pairs = [(i, (i + 2 * step) % tp_size) for i in range(tp_size)]
    return lax.ppermute(x, "tp", pairs)


def expert_rows(rows, expert_gate, expert_up, expert_down):
    gate_values = jnp.einsum("secd,edf->secf", rows, expert_gate, preferred_element_type=jnp.float32)
    up_values = jnp.einsum("secd,edf->secf", rows, expert_up, preferred_element_type=jnp.float32)
    active = (jax.nn.silu(gate_values) * up_values).astype(jnp.bfloat16)
    return jnp.einsum(
        "secf,efd->secd", active, expert_down, preferred_element_type=jnp.float32
    ).astype(jnp.bfloat16)


def expert_ring(arrived, expert_gate, expert_up, expert_down):
    chips = lax.axis_size("tp") // 2
    half = arrived.shape[0] // 2
    upward, downward = arrived[:half], arrived[half:]
    pieces = [(upward, downward)]
    for _ in range(chips - 1):
        upward, downward = hop(upward, 1), hop(downward, -1)
        pieces.append((upward, downward))

    def pair_sum(piece):
        own = jnp.concatenate(piece, axis=0)
        result = expert_rows(
            jnp.concatenate([own, hop(own, 0)], axis=0), expert_gate, expert_up, expert_down
        )
        mine, other = result[: 2 * half], result[2 * half :]
        total = mine.astype(jnp.float32) + hop(other, 0).astype(jnp.float32)
        return total[:half], total[half:]

    up_sum, down_sum = None, None
    for piece in pieces[1:] + pieces[:1]:
        up_part, down_part = pair_sum(piece)
        if up_sum is not None:
            up_part = up_part + hop(up_sum, 1).astype(jnp.float32)
            down_part = down_part + hop(down_sum, -1).astype(jnp.float32)
        up_sum, down_sum = up_part.astype(jnp.bfloat16), down_part.astype(jnp.bfloat16)
    return jnp.concatenate([up_sum, down_sum], axis=0)


def local(
    residual,
    wide_query,
    narrow_query,
    wide_keys,
    narrow_keys,
    wide_values,
    narrow_values,
    wide_query_gain,
    wide_key_gain,
    narrow_query_gain,
    narrow_key_gain,
    wide_out,
    narrow_out,
    first_gain,
    first_bias,
    route_ids,
    route_weights,
    expert_gate,
    expert_up,
    expert_down,
    shared_gate,
    shared_up,
    shared_down,
    second_gain,
    second_bias,
):
    seg_rows = wide_query.shape[0]
    position = lax.axis_index("sp") % SEQ_SHARDS * seg_rows + jnp.arange(seg_rows, dtype=jnp.int32)
    wide_rotated, wide_pack = prepare(
        wide_query,
        wide_keys,
        wide_values,
        wide_query_gain,
        wide_key_gain,
        WIDE_HEADS,
        WIDE_GROUPS,
        position,
    )
    narrow_rotated, narrow_pack = prepare(
        narrow_query,
        narrow_keys,
        narrow_values,
        narrow_query_gain,
        narrow_key_gain,
        NARROW_HEADS,
        NARROW_GROUPS,
        position,
    )
    gathered = jnp.concatenate([wide_pack, narrow_pack], axis=1)
    for level in range(SEQ_SHARDS.bit_length() - 1):
        partner = swapped(gathered, "sp", level)
        is_upper = lax.axis_index("sp") // 2**level % 2 == 1
        gathered = jnp.where(
            is_upper,
            jnp.concatenate([partner, gathered], axis=0),
            jnp.concatenate([gathered, partner], axis=0),
        )
    wide_size = wide_query_gain.shape[0]
    narrow_size = narrow_query_gain.shape[0]
    narrow_start = 2 * wide_size
    wide_mixed = attend_local(
        wide_rotated, gathered[:, :wide_size], gathered[:, wide_size:narrow_start]
    )
    narrow_mixed = attend_local(
        narrow_rotated,
        gathered[:, narrow_start : narrow_start + narrow_size],
        gathered[:, narrow_start + narrow_size :],
    )
    wide_tokens, narrow_tokens = (
        lax.all_to_all(wide_mixed, "tp", split_axis=0, concat_axis=1, tiled=True),
        lax.all_to_all(narrow_mixed, "tp", split_axis=0, concat_axis=1, tiled=True),
    )
    running = jnp.dot(
        wide_tokens,
        lax.all_gather(wide_out, "tp", axis=0, tiled=True),
        preferred_element_type=jnp.float32,
    )
    projected = running + jnp.dot(
        narrow_tokens,
        lax.all_gather(narrow_out, "tp", axis=0, tiled=True),
        preferred_element_type=jnp.float32,
    )
    hidden = layer_norm(ALPHA * residual.astype(jnp.float32) + projected, first_gain, first_bias)
    device_rows = hidden.shape[0]
    model_width = hidden.shape[1]
    sp_size = lax.axis_size("sp")
    top_count = route_ids.shape[1]
    experts = LOCAL_EXPERTS * sp_size
    capacity = max(2, (5 * device_rows * top_count + 4 * experts - 1) // (4 * experts))
    flat_ids = route_ids.reshape(-1)
    expert_hits = (flat_ids[:, None] == jnp.arange(experts, dtype=jnp.int32)[None, :]).astype(
        jnp.int32
    )
    earlier = jnp.sum((jnp.cumsum(expert_hits, axis=0) - expert_hits) * expert_hits, axis=1)
    slot_index = flat_ids * capacity + earlier
    chosen = (
        slot_index[:, None] == jnp.arange(experts * capacity, dtype=jnp.int32)[None, :]
    ).astype(jnp.float32)
    chosen = chosen.reshape(device_rows, top_count, experts * capacity)
    placing = jnp.sum(chosen, axis=1).astype(jnp.bfloat16)
    mixing = jnp.sum(chosen * route_weights[:, :, None], axis=1)
    outgoing = jnp.einsum("rs,rd->sd", placing, hidden, preferred_element_type=jnp.float32).astype(
        jnp.bfloat16
    )
    outgoing = outgoing.reshape(sp_size, LOCAL_EXPERTS, capacity, model_width)
    arrived = lax.all_to_all(outgoing, "sp", split_axis=0, concat_axis=0, tiled=True)
    summed = expert_ring(arrived, expert_gate, expert_up, expert_down)
    returned = lax.all_to_all(summed, "sp", split_axis=0, concat_axis=0, tiled=True)
    routed = jnp.dot(
        mixing,
        returned.reshape(-1, model_width).astype(jnp.float32),
        precision=lax.Precision.HIGHEST,
    )
    shared_gate_values = jnp.dot(hidden, shared_gate, preferred_element_type=jnp.float32)
    shared_up_values = jnp.dot(hidden, shared_up, preferred_element_type=jnp.float32)
    shared_active = (jax.nn.silu(shared_gate_values) * shared_up_values).astype(jnp.bfloat16)
    shared_output = jnp.dot(shared_active, shared_down, preferred_element_type=jnp.float32)
    return layer_norm(
        ALPHA * hidden.astype(jnp.float32) + routed + shared_output, second_gain, second_bias
    )


def solution(mesh):
    in_specs = (
        P(("sp", "tp"), None),
        P("sp", "tp"),
        P("sp", "tp"),
        P("sp", None),
        P("sp", None),
        P("sp", None),
        P("sp", None),
        P(),
        P(),
        P(),
        P(),
        P("tp", None),
        P("tp", None),
        P(),
        P(),
        P(("sp", "tp"), None),
        P(("sp", "tp"), None),
        P("sp", None, "tp"),
        P("sp", None, "tp"),
        P("sp", "tp", None),
        P(),
        P(),
        P(),
        P(),
        P(),
    )
    out_specs = P(("sp", "tp"), None)
    return jax.shard_map(local, mesh=mesh, in_specs=in_specs, out_specs=out_specs, check_vma=False)
```
